512 devices in a mesh: sp: 16 (over z), dp: 32 (over y, x, core).
Axes of the slice: x: 4, y: 4, z: 16, core: 2. Of those that a mesh axis runs over, the one named last changes fastest.
Arguments:
- tokens: bfloat16 [32, 2048, 2048], P('dp', 'sp'), may hold values from -6 to 6
- receptance_weight: bfloat16 [2048, 1024], P('dp'), may hold values from -0.125 to 0.125
- key_projection_weight: bfloat16 [2048, 1024], P('dp'), may hold values from -0.125 to 0.125
- value_projection_weight: bfloat16 [2048, 1024], P('dp'), may hold values from -0.125 to 0.125
- decay_down_weight: bfloat16 [2048, 256], P('dp'), may hold values from -0.125 to 0.125
- decay_up_weight: bfloat16 [2, 128, 1024], replicated, may hold values from -0.71875 to 0.71875
- decay_floor_level: float32 [2, 1024], replicated, may hold values from -10 to -2.25
- correction_rate_logit: float32 [2, 1024], P(None, 'sp'), may hold values from -4 to 4
- diagonal_address_factor: float32 [2, 1024], P(None, 'sp'), may hold values from -1 to 1
- head_norm_gain: float32 [1024], P('sp'), may hold values from 0.1 to 1.9
Outputs:
- mixed: bfloat16 [32, 2048, 1024], P('dp', 'sp')
The draws below stay inside these ranges and needn't reach their ends.
All inputs are finite; a program needn't handle non-finite values.
Results may differ from the reference program's by a relative error of at most 0.0056.
The reference program's roundings to bfloat16 on the way (of `lowered` and `pre`) count: a program that leaves them out, or rounds other values in their place, can miss the bound.
Values may be sent and summed in bfloat16 or wider, within the bound.
No kernel may reach another device: no remote copies, remote signals or barrier semaphores. Data moves between devices by JAX's collectives and lax.ppermute only.
A program may use at most 128 MiB of HBM per device.

```python
import math
import jax
import jax.numpy as jnp
from jax import lax

D = 2048
ATTENTION_SPLITS = 16
SUBSPACE_SIZE = 64
RANK = 128
CHANNEL_COUNT = 1024
LENGTH = 2048
SEQS = 32


def draw_decay_floor_level(key, part):
    first, second, third, fourth = jax.random.split(key, 4)
    keep = 5
    slow = jax.random.randint(first, (2, ATTENTION_SPLITS, 1), 0, 10) < keep
    slow_level = jax.random.uniform(second, (2, ATTENTION_SPLITS, 1), jnp.float32, -9.5, -8.5)
    fast_level = jax.random.uniform(third, (2, ATTENTION_SPLITS, 1), jnp.float32, -3.25, -2.75)
    jitter = jax.random.uniform(fourth, (2, ATTENTION_SPLITS, SUBSPACE_SIZE), jnp.float32, -0.5, 0.5)
    return (jnp.where(slow, slow_level, fast_level) + jitter).reshape(2, ATTENTION_SPLITS * SUBSPACE_SIZE)


def level_of(stream_key, shape, cuts, low, high):
    loudness = 1.0
    for axis_at, parts in cuts:
        heights = jax.random.uniform(jax.random.fold_in(jax.random.fold_in(stream_key, 6), axis_at), (parts,), jnp.float32, low / len(cuts), high / len(cuts))
        loudness = loudness * jnp.repeat(jnp.exp(heights), shape[axis_at] // parts).reshape((-1,) + (1,) * (len(shape) - 1 - axis_at))
    return loudness


def gaussian(own_key, dims, scale, limit, cuts=(), dtype=jnp.bfloat16):
    entries = scale * jax.random.normal(own_key, dims, jnp.float32)
    if cuts:
        entries = entries * level_of(own_key, dims, cuts, -0.22, 0.18)
    return jnp.clip(entries, -limit, limit).astype(dtype)


def setup_inputs(seed: int = 0) -> dict:
    splits = jax.random.split(jax.random.key(seed), 11)
    tokens = gaussian(splits[0], (SEQS, LENGTH, D), 1.0, 6.0, ((0, 32), (1, 16)))
    receptance_weight = gaussian(splits[1], (D, CHANNEL_COUNT), D ** -0.5, 0.125, ((0, 32),))
    key_projection_weight = gaussian(splits[2], (D, CHANNEL_COUNT), D ** -0.5, 0.125, ((0, 32),))
    value_projection_weight = gaussian(splits[3], (D, CHANNEL_COUNT), D ** -0.5, 0.125, ((0, 32),))
    decay_down_weight = gaussian(splits[4], (D, 2 * RANK), D ** -0.5, 0.125, ((0, 32),))
    decay_up_weight = gaussian(splits[5], (2, RANK, CHANNEL_COUNT), 0.12, 0.71875)
    decay_floor_level = draw_decay_floor_level(jax.random.fold_in(splits[10], 71), 0)
    correction_rate_logit = gaussian(splits[7], (2, CHANNEL_COUNT), 1.0, 4.0, ((1, 16),), jnp.float32)
    diagonal_address_factor = gaussian(splits[8], (2, CHANNEL_COUNT), 0.2, 1.0, ((1, 16),), jnp.float32)
    head_norm_gain = jnp.clip(1.0 + 0.18 * jax.random.normal(splits[9], (CHANNEL_COUNT,), jnp.float32), 0.1, 1.9)
    return {"tokens": tokens, "receptance_weight": receptance_weight, "key_projection_weight": key_projection_weight, "value_projection_weight": value_projection_weight, "decay_down_weight": decay_down_weight, "decay_up_weight": decay_up_weight, "decay_floor_level": decay_floor_level, "correction_rate_logit": correction_rate_logit, "diagonal_address_factor": diagonal_address_factor, "head_norm_gain": head_norm_gain}


def contract(pattern, former, latter):
    return jnp.einsum(pattern, former, latter, precision=lax.Precision.HIGHEST)

def recur(state, inputs):
    query, rated_key, value, eraser, writer, decay = inputs
    pulled = contract('hij,hj->hi', state, eraser)
    state = state * decay[:, None, :] + pulled[:, :, None] * writer[:, None, :] + value[:, :, None] * rated_key[:, None, :]
    return (state, contract('hij,hj->hi', state, query))

def reference(tokens, receptance_weight, key_projection_weight, value_projection_weight, decay_down_weight, decay_up_weight, decay_floor_level, correction_rate_logit, diagonal_address_factor, head_norm_gain):
    flat = tokens.reshape(SEQS * LENGTH, D)
    receive = jnp.dot(flat, receptance_weight, preferred_element_type=jnp.float32).astype(jnp.bfloat16)
    key_rows = jnp.dot(flat, key_projection_weight, preferred_element_type=jnp.float32).astype(jnp.bfloat16)
    value_rows = jnp.dot(flat, value_projection_weight, preferred_element_type=jnp.float32).astype(jnp.bfloat16)
    lowered = jnp.tanh(jnp.dot(flat, decay_down_weight, preferred_element_type=jnp.float32)).astype(jnp.bfloat16)
    forward_pre = (jnp.dot(lowered[:, :RANK], decay_up_weight[0], preferred_element_type=jnp.float32) + decay_floor_level[0]).astype(jnp.bfloat16)
    backward_pre = (jnp.dot(lowered[:, RANK:], decay_up_weight[1], preferred_element_type=jnp.float32) + decay_floor_level[1]).astype(jnp.bfloat16)
    amend_strength = jax.nn.sigmoid(correction_rate_logit).reshape(2, ATTENTION_SPLITS, SUBSPACE_SIZE)
    diagonal_extra = diagonal_address_factor.reshape(2, ATTENTION_SPLITS, SUBSPACE_SIZE)
    gain = head_norm_gain.reshape(ATTENTION_SPLITS, SUBSPACE_SIZE)

    def to_sequences(content_matrix_full):
        return content_matrix_full.reshape(SEQS, LENGTH, ATTENTION_SPLITS, SUBSPACE_SIZE)

    def one_sequence(items):
        probe_matrix_full, keys, content_matrix_full, fore, backs = [piece.astype(jnp.float32) for piece in items]
        normed = keys / jnp.sqrt(lax.optimization_barrier(jnp.sum(keys * keys, -1, keepdims=True)) + 1.0)
        total = jnp.zeros((LENGTH, ATTENTION_SPLITS, SUBSPACE_SIZE), jnp.float32)
        for sweep_orientation, pre in ((0, fore), (1, backs)):
            decay = jnp.exp(-math.exp(-0.5) * jax.nn.sigmoid(pre))
            strength_multiplied = keys * amend_strength[sweep_orientation]
            inputs = (probe_matrix_full, strength_multiplied, content_matrix_full, -normed, normed * amend_strength[sweep_orientation], decay)
            if sweep_orientation == 1:
                inputs = tuple((jnp.flip(piece, 0) for piece in inputs))
            state = jnp.zeros((ATTENTION_SPLITS, SUBSPACE_SIZE, SUBSPACE_SIZE), jnp.float32)
            _, readout = lax.scan(recur, state, inputs)
            if sweep_orientation == 1:
                readout = jnp.flip(readout, 0)
            centred = readout - lax.optimization_barrier(jnp.mean(readout, -1, keepdims=True))
            variance = lax.optimization_barrier(jnp.mean(centred * centred, -1, keepdims=True))
            diagonal_contribution = lax.optimization_barrier(jnp.sum(probe_matrix_full * strength_multiplied * diagonal_extra[sweep_orientation], -1, keepdims=True)) * content_matrix_full
            total = total + (centred * lax.rsqrt(variance + 0.00064) * gain + diagonal_contribution)
        return total.reshape(LENGTH, ATTENTION_SPLITS * SUBSPACE_SIZE).astype(jnp.bfloat16)
    return lax.map(one_sequence, (to_sequences(receive), to_sequences(key_rows), to_sequences(value_rows), to_sequences(forward_pre), to_sequences(backward_pre)))
```

```python
import math
import functools
import jax
import jax.numpy as jnp
from jax import lax
from jax.experimental import pallas as pl
from jax.experimental.pallas import tpu as pltpu
from jax.sharding import PartitionSpec as P

BF = jnp.bfloat16
F32 = jnp.float32
C = 128
H = 64


def split2(x):
    hi = x.astype(BF)
    return hi, (x - hi.astype(F32)).astype(BF)


def left3(a):
    hi, lo = split2(a)
    return jnp.concatenate([hi, lo], 1)


def right3(b):
    hi, lo = split2(b)
    return jnp.concatenate(
        [jnp.concatenate([hi, lo], 1), jnp.concatenate([hi, jnp.zeros_like(lo)], 1)], 0
    )


def dot3(a3, b3):
    t = jnp.dot(a3, b3, preferred_element_type=F32)
    n = t.shape[1] // 2
    return t[:, :n] + t[:, n:]


def nt(a, b):
    return lax.dot_general(a, b, (((1,), (1,)), ((), ())), preferred_element_type=F32)


def tn(a, b):
    return lax.dot_general(a, b, (((0,), (0,)), ((), ())), preferred_element_type=F32)


def head_ones(scale=1.0):
    r = lax.broadcasted_iota(jnp.int32, (256, 128), 0)
    c = lax.broadcasted_iota(jnp.int32, (256, 128), 1)
    return jnp.where(((r >> 6) & 1) == (c >> 6), scale, 0.0).astype(BF)


def head_sum(x, ones):
    hi, lo = split2(x)
    return jnp.dot(jnp.concatenate([hi, lo], 1), ones, preferred_element_type=F32)


def product(a, b):
    return dot3(left3(a), right3(b))


def prep_kernel(q_ref, k_ref, v_ref, low_ref, up_ref, floor_ref, rate_ref, msg_ref, y_ref, qx_ref):
    chunks = q_ref.shape[0] // C
    q = q_ref[...].astype(F32)
    k = k_ref[...].astype(F32)
    v = v_ref[...].astype(F32)
    row = lax.broadcasted_iota(jnp.int32, (C, C), 0)
    col = lax.broadcasted_iota(jnp.int32, (C, C), 1)
    x = row ^ col
    left = lax.broadcasted_iota(jnp.int32, (C, C), 1) < H
    ones = head_ones()
    inv = 1.0 / (1.0 + head_sum(k * k, ones))
    nk = -(k * inv)
    probs = []
    for d in range(2):
        pre = (
            jnp.dot(low_ref[:, d * 128 : (d + 1) * 128], up_ref[d], preferred_element_type=F32)
            + floor_ref[d : d + 1, :]
        ).astype(BF).astype(F32)
        logd = -math.exp(-0.5) * jax.nn.sigmoid(pre)
        rate = jax.nn.sigmoid(rate_ref[d : d + 1, :])
        kap = k * rate
        strict = (col < row) if d == 0 else (col > row)
        tri = jnp.where((col <= row) if d == 0 else (col >= row), 1.0, 0.0).astype(BF)
        for ci in range(chunks):
            c = ci if d == 0 else chunks - 1 - ci
            sl = slice(c * C, (c + 1) * C)
            ld = logd[sl]
            hi, lo = split2(ld)
            cs = jnp.dot(tri, jnp.concatenate([hi, lo], 1), preferred_element_type=F32)
            inc = cs[:, :128] + cs[:, 128:]
            mid = inc[C // 2 : C // 2 + 1]
            fin = inc[C - 1 : C] if d == 0 else inc[0:1]
            rel = inc - mid
            up_e = jnp.exp(rel)
            gq = nk[sl] * jnp.exp(rel - ld)
            rq = q[sl] * up_e
            pk = kap[sl] * jnp.exp(-rel)
            emid = jnp.exp(mid)
            ke = pk * jnp.exp(fin - mid)
            g0 = gq * emid
            r0 = rq * emid
            gl = pltpu.roll(g0, H, 1)
            vs = v[sl]
            pkh, pkl = split2(pk)
            rhs = jnp.concatenate(
                [jnp.concatenate([pkh, pkh], 1), jnp.concatenate([pkl, jnp.zeros_like(pkl)], 1)], 0
            )
            zero = jnp.zeros_like(gq)
            att = nt(
                jnp.concatenate(
                    [
                        left3(jnp.where(left, gq, zero)),
                        left3(jnp.where(left, rq, zero)),
                        left3(jnp.where(left, zero, gq)),
                        left3(jnp.where(left, zero, rq)),
                    ],
                    0,
                ),
                rhs,
            )
            att = att[:, :C] + att[:, C:]
            heads = []
            for a in range(2):
                m = jnp.where(strict, att[2 * a * C : (2 * a + 1) * C], 0.0)
                r = jnp.where(tri > 0, att[(2 * a + 1) * C : (2 * a + 2) * C], 0.0)
                b = jnp.where(left, vs, gl) if a == 0 else jnp.where(left, gl, vs)
                heads.append(dict(m=m, r=r, b=b))
            probs.append(
                dict(d=d, c=c, heads=heads, ke=ke, r0=r0, fin=fin)
            )
    allh = [h for p in probs for h in p["heads"]]
    for h in allh:
        h["n"] = jnp.where(x == 1, h["m"], 0.0)
    for lb in range(1, 7):
        sel = (x >> lb) == 1
        for h in allh:
            h["off"] = jnp.where(sel, h["m"], 0.0)
            h["w"] = h["off"] + product(h["off"], h["n"])
        for h in allh:
            h["n"] = h["n"] + h["w"] + product(h["n"], h["w"])
    for h in allh:
        h["x"] = h["b"] + dot3(left3(h["n"]), right3(h["b"]))
    row2 = lax.broadcasted_iota(jnp.int32, (C, C), 0)
    for d in range(2):
        u = None
        for ci in range(chunks):
            p = probs[d * chunks + ci]
            sl = slice(p["c"] * C, (p["c"] + 1) * C)
            xa, xb = p["heads"][0]["x"], p["heads"][1]["x"]
            ya = dot3(left3(p["heads"][0]["r"]), right3(xa))
            yb = dot3(left3(p["heads"][1]["r"]), right3(xb))
            y0 = jnp.where(left, ya, yb)
            qx = p["r0"] + pltpu.roll(jnp.where(left, yb, ya), H, 1)
            kh, kl = split2(
                jnp.concatenate([jnp.where(left, p["ke"], 0.0), jnp.where(left, 0.0, p["ke"])], 0)
            )
            xh, xl = split2(jnp.concatenate([xa, xb], 0))
            un = tn(kh, jnp.concatenate([xh, xl], 1))
            un = un[:, :C] + un[:, C:] + tn(kl, xh)
            un = jnp.where(row2 < H, un, pltpu.roll(un, H, 1))
            ef = jnp.exp(p["fin"])
            efr = pltpu.roll(jnp.broadcast_to(ef, (C, C)), H, 1)
            dm = jnp.where(row2 < H, efr, jnp.broadcast_to(ef, (C, C)))
            un = un + jnp.where(col == (row2 & (H - 1)) + H, dm, 0.0)
            if u is None:
                u = un
            else:
                uh, ul = split2(u)
                ub_i = jnp.where(row2 < H, jnp.where(left, u, 0.0), jnp.where(left, 0.0, pltpu.roll(u, H, 1)))
                ub_t = jnp.where(row2 < H, jnp.where(left, pltpu.roll(u, H, 1), 0.0), jnp.where(left, 0.0, u))
                bh, bl = split2(jnp.concatenate([ub_i, ub_t], 1))
                q3 = left3(qx)
                qd = jnp.dot(
                    q3, jnp.concatenate([bh, bh], 0), preferred_element_type=F32
                ) + jnp.dot(q3[:, :C], bl, preferred_element_type=F32)
                y0 = y0 + qd[:, :C]
                qx = qd[:, C:]
                tl = jnp.where(left, 0.0, un)
                t2 = jnp.where(row2 < H, jnp.where(left, pltpu.roll(un, H, 1), 0.0), tl)
                th, tlo = split2(t2)
                lhs = jnp.concatenate([th, tlo], 1)
                comp = (
                    jnp.dot(lhs, jnp.concatenate([uh, uh], 0), preferred_element_type=F32)
                    + jnp.dot(th, ul, preferred_element_type=F32)
                )
                u = comp + jnp.where(left, un, 0.0)
            y_ref[d, sl, :] = y0
            qx_ref[d, sl, :] = qx
        msg_ref[d] = u[:H].astype(BF)
        msg_ref[2 + d] = u[H:].astype(BF)


def prep(qkv, low, up, floor, rate, tokens):
    rows, width3 = qkv.shape
    width = width3 // 3
    seqs = rows // tokens
    hps = width // 128
    grid = (seqs, hps)
    sb = lambda off: pl.BlockSpec((tokens, 128), lambda s, h: (s, h + off * hps))
    return pl.pallas_call(
        prep_kernel,
        grid=grid,
        in_specs=[
            sb(0),
            sb(1),
            sb(2),
            pl.BlockSpec((tokens, 256), lambda s, h: (s, 0)),
            pl.BlockSpec((2, 128, 128), lambda s, h: (0, 0, h)),
            pl.BlockSpec((2, 128), lambda s, h: (0, h)),
            pl.BlockSpec((2, 128), lambda s, h: (0, h)),
        ],
        out_specs=[
            pl.BlockSpec((4, H, 128), lambda s, h: (s * hps + h, 0, 0)),
            pl.BlockSpec((2, tokens, 128), lambda s, h: (0, s, h)),
            pl.BlockSpec((2, tokens, 128), lambda s, h: (0, s, h)),
        ],
        out_shape=[
            jax.ShapeDtypeStruct((seqs * hps * 4, H, 128), BF),
            jax.ShapeDtypeStruct((2, rows, width), F32),
            jax.ShapeDtypeStruct((2, rows, width), F32),
        ],
        compiler_params=pltpu.CompilerParams(vmem_limit_bytes=56 * 1024 * 1024),
        name="prep",
    )(qkv, qkv, qkv, low, up, floor, rate)


def final_kernel(y_ref, qx_ref, s_ref, q_ref, k_ref, v_ref, rate_ref, diag_ref, gain_ref, o_ref):
    q = q_ref[...].astype(F32)
    k = k_ref[...].astype(F32)
    v = v_ref[...].astype(F32)
    mean = head_ones(1.0 / H)
    ones = head_ones()
    wt = jax.nn.sigmoid(rate_ref[0:1]) * diag_ref[0:1] + jax.nn.sigmoid(rate_ref[1:2]) * diag_ref[1:2]
    own = head_sum(q * k * wt, ones) * v
    total = own
    z = jnp.zeros((H, H), BF)
    for d in range(2):
        sa, sb = s_ref[d], s_ref[2 + d]
        blk = jnp.concatenate(
            [
                jnp.concatenate([jnp.concatenate([sa[:, :H], sa[:, H:]], 0), z], 1),
                jnp.concatenate([z, jnp.concatenate([sb[:, :H], sb[:, H:]], 0)], 1),
            ],
            0,
        )
        y = y_ref[d] + jnp.dot(
            left3(qx_ref[d]), jnp.concatenate([blk, blk], 0), preferred_element_type=F32
        )
        cen = y - head_sum(y, mean)
        var = head_sum(cen * cen, mean)
        total = total + cen * lax.rsqrt(var + 0.00064) * gain_ref[...]
    o_ref[...] = total.astype(BF)


def final(y, qx, s, qkv, rate, diag, gain, tokens):
    rows, width3 = qkv.shape
    width = width3 // 3
    seqs = rows // tokens
    hps = width // 128
    sb = lambda off: pl.BlockSpec((tokens, 128), lambda s, h: (s, h + off * hps))
    dspec = pl.BlockSpec((2, tokens, 128), lambda s, h: (0, s, h))
    par = pl.BlockSpec((2, 128), lambda s, h: (0, h))
    return pl.pallas_call(
        final_kernel,
        grid=(seqs, hps),
        in_specs=[
            dspec,
            dspec,
            pl.BlockSpec((4, 32, 128), lambda s, h: (s * hps + h, 0, 0)),
            sb(0),
            sb(1),
            sb(2),
            par,
            par,
            pl.BlockSpec((1, 128), lambda s, h: (0, h)),
        ],
        out_specs=pl.BlockSpec((tokens, 128), lambda s, h: (s, h)),
        out_shape=jax.ShapeDtypeStruct((rows, width), BF),
        compiler_params=pltpu.CompilerParams(vmem_limit_bytes=56 * 1024 * 1024),
        name="final",
    )(y, qx, s, qkv, qkv, qkv, rate, diag, gain)


def scan_kernel(roles, back_ref, u_ref, o_ref):
    groups = u_ref.shape[0] // roles
    back = back_ref[0]
    states = [jnp.zeros((H, H), F32) for _ in range(roles)]
    zero = jnp.zeros((H, 128), BF)
    for i in range(groups):
        g = jnp.where(back == 1, groups - 1 - i, i)
        for p in range(roles):
            src = g * roles + p
            s = states[p]
            hi, lo = split2(s)
            o_ref[src] = jnp.concatenate([hi[:32], hi[32:]], 1)
            u = u_ref[src]
            t = jnp.dot(
                u, jnp.concatenate([zero, jnp.concatenate([hi, lo], 1)], 0), preferred_element_type=F32
            )
            states[p] = u[:, :H].astype(F32) + t[:, :H] + t[:, H:]


def scan_states(u, back, roles):
    n = u.shape[0]
    return pl.pallas_call(
        functools.partial(scan_kernel, roles),
        in_specs=[pl.BlockSpec(memory_space=pltpu.SMEM), pl.BlockSpec(memory_space=pltpu.VMEM)],
        out_specs=pl.BlockSpec(memory_space=pltpu.VMEM),
        out_shape=jax.ShapeDtypeStruct((n, 32, 128), BF),
        name="states",
    )(back, u)


def project_kernel(
    idx_ref, b0, fm, fp, ot, ob, r1, r2, r3t, r3b, t0, t1, t2, t3, qkv_ref, low_ref, w_ref
):
    rows = b0.shape[0]
    half = rows // 2
    w_ref[idx_ref[0]] = b0[...]
    w_ref[idx_ref[1]] = fm[...]
    w_ref[idx_ref[2]] = fp[...]
    w_ref[idx_ref[3], :half] = ot[...]
    w_ref[idx_ref[3], half:] = ob[...]
    for i in range(4):
        w_ref[idx_ref[4 + i]] = r1[i * rows : (i + 1) * rows]
        w_ref[idx_ref[8 + i]] = r2[i * rows : (i + 1) * rows]
    for i in range(2):
        w_ref[idx_ref[12 + i]] = r3t[i * rows : (i + 1) * rows]
        w_ref[idx_ref[14 + i]] = r3b[i * rows : (i + 1) * rows]
    width3 = qkv_ref.shape[1]
    n = t0.shape[0]
    for i, t in enumerate((t0, t1, t2, t3)):
        at = pl.ds(pl.multiple_of(idx_ref[16 + i] * n, n), n)
        w = w_ref[...].reshape(-1, w_ref.shape[2])
        out = jnp.dot(t[...], w, preferred_element_type=F32)
        qkv_ref[at, :] = out[:, :width3].astype(BF)
        low_ref[at, :] = jnp.tanh(out[:, width3:]).astype(BF)


def project(idx, blocks, toks, width3):
    cols = blocks[0].shape[1]
    n = toks[0].shape[0]
    vm = pl.BlockSpec(memory_space=pltpu.VMEM)
    return pl.pallas_call(
        project_kernel,
        in_specs=[pl.BlockSpec(memory_space=pltpu.SMEM)] + [vm] * 13,
        out_specs=[vm, vm],
        out_shape=[
            jax.ShapeDtypeStruct((4 * n, width3), BF),
            jax.ShapeDtypeStruct((4 * n, cols - width3), BF),
        ],
        scratch_shapes=[pltpu.VMEM((16, blocks[0].shape[0], cols), BF)],
        compiler_params=pltpu.CompilerParams(vmem_limit_bytes=56 * 1024 * 1024),
        name="project",
    )(idx, *blocks, *toks)


def shift(first, by):
    pairs = []
    for i in range(32):
        core, j = i % 2, i // 2
        y, x = j // 4, j % 4
        if (core == 0) == first:
            x = (x + by) % 4
        else:
            y = (y + by) % 4
        pairs.append((i, (y * 4 + x) * 2 + core))
    return pairs


CORES = [(i, i ^ 1) for i in range(32)]
ZPAIRS = [(i, i ^ 1) for i in range(16)]


def body(tokens, wq, wk, wv, wd, up, floor, rate, diag, gain):
    z = lax.axis_index("sp")
    dp = lax.axis_index("dp")
    c, p = dp % 2, z % 2
    j = dp // 2
    y, x = j // 4, j % 4
    width = 256
    tok = tokens.reshape(-1, tokens.shape[2])
    n = tok.shape[0]

    def columns(role):
        cut = lambda w: lax.dynamic_slice_in_dim(w, role * width, width, 1)
        return jnp.concatenate([cut(wq), cut(wk), cut(wv), wd], 1)

    role = 2 * p + c
    keep = columns(role)
    recv = lax.ppermute(columns(2 * p + 1 - c), "dp", CORES)
    b0 = jnp.where(c == 0, jnp.concatenate([keep, recv], 0), jnp.concatenate([recv, keep], 0))
    rows = b0.shape[0]
    fm = lax.ppermute(b0, "dp", shift(True, 1))
    fp = lax.ppermute(b0, "dp", shift(True, -1))
    ot = lax.ppermute(fm[: rows // 2], "dp", shift(True, 1))
    ob = lax.ppermute(fp[rows // 2 :], "dp", shift(True, -1))
    tz = lax.ppermute(tok, "sp", ZPAIRS)
    tc = lax.ppermute(tok, "dp", CORES)
    s4 = jnp.concatenate([b0, fm, fp, ot, ob], 0)
    r1 = lax.ppermute(s4, "dp", shift(False, 1))
    r2 = lax.ppermute(s4, "dp", shift(False, -1))
    tcz = lax.ppermute(tz, "dp", CORES)
    r3t = lax.ppermute(r1[: 2 * rows], "dp", shift(False, 1))
    r3b = lax.ppermute(r2[2 * rows :], "dp", shift(False, -1))

    par = jnp.concatenate([rate, diag, gain[None], jnp.zeros((3, gain.shape[0]), F32)], 0)
    par = jnp.broadcast_to(par[None], (16,) + par.shape)
    par = lax.all_to_all(par, "sp", split_axis=0, concat_axis=0, tiled=True)
    par = lax.dynamic_slice_in_dim(par, 4 * role, 4, 0)
    par = jnp.transpose(par, (1, 0, 2)).reshape(8, width)
    rate4, diag4, gain4 = par[0:2], par[2:4], par[4:5]
    up4 = lax.dynamic_slice_in_dim(up, role * width, width, 2)
    floor4 = lax.dynamic_slice_in_dim(floor, role * width, width, 1)

    a = jnp.where(c == 0, x, y)
    b = jnp.where(c == 0, y, x)
    ids = []
    for eps in (0, -1, 1, 2):
        for delta in (0, -1, 1, 2):
            aa, bb = (a + delta) % 4, (b + eps) % 4
            ids.append(jnp.where(c == 0, bb * 4 + aa, aa * 4 + bb))
    ids += [2 * c + p, 2 * c + 1 - p, 2 * (1 - c) + p, 2 * (1 - c) + 1 - p]
    idx = jnp.stack(ids).astype(jnp.int32)
    qkv, low = project(
        idx, (b0, fm, fp, ot, ob, r1, r2, r3t, r3b), (tok, tz, tc, tcz), 3 * width
    )
    span = 2 * n
    msg, y0, qx = prep(qkv, low, up4, floor4, rate4, span)
    got = lax.all_to_all(msg, "sp", split_axis=0, concat_axis=0, tiled=True)
    st = scan_states(got, (z % 2).reshape(1).astype(jnp.int32), 2)
    st = lax.all_to_all(st, "sp", split_axis=0, concat_axis=0, tiled=True)
    out = final(y0, qx, st, qkv, rate4, diag4, gain4, span)

    out = out.reshape(2, 2, n, width)
    mine = lax.dynamic_index_in_dim(out, p, 1, False)
    rz = lax.ppermute(lax.dynamic_index_in_dim(out, 1 - p, 1, False), "sp", ZPAIRS)
    pick = lambda m, s: lax.dynamic_index_in_dim(m, s, 0, False)
    low_p = jnp.where(p == 0, mine, rz)
    high_p = jnp.where(p == 0, rz, mine)
    both = jnp.concatenate([low_p, high_p], 2)
    far = lax.ppermute(pick(both, 1 - c), "dp", CORES)
    near = pick(both, c)
    first = jnp.where(c == 0, near, far)
    second = jnp.where(c == 0, far, near)
    res = jnp.concatenate(
        [first[:, :width], second[:, :width], first[:, width:], second[:, width:]], 1
    )
    return res.reshape(1, n, 4 * width)


def solution(mesh):
    in_specs = (
        P("dp", "sp", None),
        P("dp", None),
        P("dp", None),
        P("dp", None),
        P("dp", None),
        P(),
        P(),
        P(None, "sp"),
        P(None, "sp"),
        P("sp"),
    )
    return jax.shard_map(
        body, mesh=mesh, in_specs=in_specs, out_specs=P("dp", "sp", None), check_vma=False
    )
```

```python
import math
import functools
import jax
import jax.numpy as jnp
from jax import lax
from jax.experimental import pallas as pl
from jax.experimental.pallas import tpu as pltpu
from jax.sharding import PartitionSpec as P

BF = jnp.bfloat16
F32 = jnp.float32
C = 128
H = 64


def split2(x):
    hi = x.astype(BF)
    return hi, (x - hi.astype(F32)).astype(BF)


def left3(a):
    hi, lo = split2(a)
    return jnp.concatenate([hi, lo], 1)


def right3(b):
    hi, lo = split2(b)
    return jnp.concatenate(
        [jnp.concatenate([hi, lo], 1), jnp.concatenate([hi, jnp.zeros_like(lo)], 1)], 0
    )


def dot3(a3, b3):
    t = jnp.dot(a3, b3, preferred_element_type=F32)
    n = t.shape[1] // 2
    return t[:, :n] + t[:, n:]


def nt(a, b):
    return lax.dot_general(a, b, (((1,), (1,)), ((), ())), preferred_element_type=F32)


def tn(a, b):
    return lax.dot_general(a, b, (((0,), (0,)), ((), ())), preferred_element_type=F32)


def head_ones(scale=1.0):
    r = lax.broadcasted_iota(jnp.int32, (256, 128), 0)
    c = lax.broadcasted_iota(jnp.int32, (256, 128), 1)
    return jnp.where(((r >> 6) & 1) == (c >> 6), scale, 0.0).astype(BF)


def head_sum(x, ones):
    hi, lo = split2(x)
    return jnp.dot(jnp.concatenate([hi, lo], 1), ones, preferred_element_type=F32)


def mm(a, b):
    return jnp.dot(a.astype(BF), b.astype(BF), preferred_element_type=F32)


def product(a, b):
    return dot3(left3(a), right3(b))


def pick_rows(x, size, off):
    return jnp.concatenate([x[i + off : i + off + size] for i in range(0, C, 2 * size)], 0)


def put_rows(rows, rest, size, off):
    parts = []
    for n, i in enumerate(range(0, C, 2 * size)):
        new = rows[n * size : (n + 1) * size]
        old = rest[i : i + size] if off else rest[i + size : i + 2 * size]
        parts += [old, new] if off else [new, old]
    return jnp.concatenate(parts, 0)


def gates(d, low, up, floor, pair):
    lanes = pl.ds(pl.multiple_of(pair * 128, 128), 128)
    pre = (
        jnp.dot(low[:, d * 128 : (d + 1) * 128], up[d, :, lanes], preferred_element_type=F32)
        + floor[d : d + 1, lanes]
    )
    return -math.exp(-0.5) * jax.nn.sigmoid(pre.astype(BF).astype(F32))


def head_row(par, pair, i):
    return jnp.concatenate([par[2 * pair, i : i + 1, :], par[2 * pair + 1, i : i + 1, :]], 1)


def sums(d, ld, tri):
    hi, lo = split2(ld)
    cs = jnp.dot(tri, jnp.concatenate([hi, lo], 1), preferred_element_type=F32)
    inc = cs[:, :128] + cs[:, 128:]
    return inc, inc[C // 2 : C // 2 + 1], inc[C - 1 : C] if d == 0 else inc[0:1]


def against(parts, pk):
    pkh, pkl = split2(pk)
    rhs = jnp.concatenate(
        [jnp.concatenate([pkh, pkh], 1), jnp.concatenate([pkl, jnp.zeros_like(pkl)], 1)], 0
    )
    att = nt(jnp.concatenate([left3(p) for p in parts], 0), rhs)
    att = att[:, :C] + att[:, C:]
    return [att[i * C : (i + 1) * C] for i in range(len(parts))]


def consts():
    row = lax.broadcasted_iota(jnp.int32, (C, C), 0)
    col = lax.broadcasted_iota(jnp.int32, (C, C), 1)
    tris = [jnp.where(m, 1.0, 0.0).astype(BF) for m in (col <= row, col >= row)]
    return row, col, row ^ col, col < H, tris


def maps_kernel(role, k_ref, v_ref, low_ref, up_ref, floor_ref, par_ref, msg_ref, x_ref, u_ref):
    chunks = k_ref.shape[0] // C
    row, col, x, left, tris = consts()
    hps = k_ref.shape[1] // 128
    probs = []
    for hp, d in [(hp, d) for hp in range(hps) for d in range(2)]:
        ln = slice(hp * 128, (hp + 1) * 128)
        k = k_ref[:, ln].astype(F32)
        v = v_ref[:, ln].astype(F32)
        nk = -(k / (1.0 + head_sum(k * k, head_ones())))
        pair = role() * hps + hp
        logd = gates(d, low_ref, up_ref, floor_ref, pair)
        kap = k * jax.nn.sigmoid(head_row(par_ref, pair, d))
        strict = (col < row) if d == 0 else (col > row)
        for ci in range(chunks):
            c = ci if d == 0 else chunks - 1 - ci
            sl = slice(c * C, (c + 1) * C)
            ld = logd[sl]
            inc, mid, fin = sums(d, ld, tris[d])
            rel = inc - mid
            gq = nk[sl] * jnp.exp(rel - ld)
            pk = kap[sl] * jnp.exp(-rel)
            ke = pk * jnp.exp(fin - mid)
            gl = pltpu.roll(gq * jnp.exp(mid), H, 1)
            vs = v[sl]
            zero = jnp.zeros_like(gq)
            att = against([jnp.where(left, gq, zero), jnp.where(left, zero, gq)], pk)
            heads = []
            for a in range(2):
                m = jnp.where(strict, att[a], 0.0)
                b = jnp.where(left, vs, gl) if a == 0 else jnp.where(left, gl, vs)
                heads.append(dict(m=m, b=b, d=d))
            probs.append(dict(d=d, c=c, heads=heads, ke=ke, fin=fin))
    allh = [h for p in probs for h in p["heads"]]
    zero = jnp.zeros((C, C), F32)
    for h in allh:
        h["n"] = jnp.where(x == 1, h["m"], 0.0)
    for lb in range(1, 7):
        size = 1 << lb
        sel = (x >> lb) == 1
        for h in allh:
            off = jnp.where(sel, h["m"], 0.0)
            if size >= 8:
                at = size if h["d"] == 0 else 0
                off = pick_rows(off, size, at)
                h["w"] = off + mm(off, h["n"])
            else:
                h["w"] = off + mm(off, h["n"])
        for h in allh:
            if size >= 8:
                at = size if h["d"] == 0 else 0
                nr = pick_rows(h["n"], size, at)
                nr = nr + h["w"] + mm(nr, put_rows(h["w"], zero, size, at))
                h["n"] = put_rows(nr, h["n"], size, at)
            else:
                h["n"] = h["n"] + h["w"] + mm(h["n"], h["w"])
    for h in allh:
        h["nb"] = h["n"].astype(BF)
        h["x"] = h["b"] + mm(h["nb"], h["b"])
    for h in allh:
        h["res"] = h["b"] - h["x"] + product(h["m"], h["x"])
    for h in allh:
        h["x"] = h["x"] + h["res"] + mm(h["nb"], h["res"])
    for hp, d in [(hp, d) for hp in range(hps) for d in range(2)]:
        u = None
        for ci in range(chunks):
            p = probs[(hp * 2 + d) * chunks + ci]
            xa, xb = p["heads"][0]["x"], p["heads"][1]["x"]
            x_ref[hp, d, p["c"], 0] = xa
            x_ref[hp, d, p["c"], 1] = xb
            kh, kl = split2(
                jnp.concatenate([jnp.where(left, p["ke"], 0.0), jnp.where(left, 0.0, p["ke"])], 0)
            )
            xh, xl = split2(jnp.concatenate([xa, xb], 0))
            un = tn(kh, jnp.concatenate([xh, xl], 1))
            un = un[:, :C] + un[:, C:] + tn(kl, xh)
            un = jnp.where(row < H, un, pltpu.roll(un, H, 1))
            ef = jnp.broadcast_to(jnp.exp(p["fin"]), (C, C))
            dm = jnp.where(row < H, pltpu.roll(ef, H, 1), ef)
            un = un + jnp.where(col == (row & (H - 1)) + H, dm, 0.0)
            if u is None:
                u = un
                u_ref[hp, d] = u
            else:
                t2 = jnp.where(
                    row < H,
                    jnp.where(left, pltpu.roll(un, H, 1), 0.0),
                    jnp.where(left, 0.0, un),
                )
                u = product(t2, u) + jnp.where(left, un, 0.0)
        msg_ref[4 * hp + d] = u[:H].astype(BF)
        msg_ref[4 * hp + 2 + d] = u[H:].astype(BF)


def outputs_kernel(
    role, q_ref, k_ref, v_ref, low_ref, up_ref, floor_ref, par_ref, x_ref, u_ref, y_ref, qx_ref, own_ref
):
    chunks = k_ref.shape[0] // C
    q = q_ref[...].astype(F32)
    k = k_ref[...].astype(F32)
    row, _, _, left, tris = consts()
    pair = role() * pl.num_programs(1) + pl.program_id(1)
    rates = [jax.nn.sigmoid(head_row(par_ref, pair, d)) for d in range(2)]
    wt = rates[0] * head_row(par_ref, pair, 2) + rates[1] * head_row(par_ref, pair, 3)
    own_ref[...] = head_sum(q * k * wt, head_ones()) * v_ref[...].astype(F32)
    for d in range(2):
        logd = gates(d, low_ref, up_ref, floor_ref, pair)
        kap = k * rates[d]
        u = u_ref[0, d]
        for ci in range(chunks):
            c = ci if d == 0 else chunks - 1 - ci
            sl = slice(c * C, (c + 1) * C)
            inc, mid, _ = sums(d, logd[sl], tris[d])
            rel = inc - mid
            rq = q[sl] * jnp.exp(rel)
            pk = kap[sl] * jnp.exp(-rel)
            zero = jnp.zeros_like(rq)
            att = against([jnp.where(left, rq, zero), jnp.where(left, zero, rq)], pk)
            ya, yb = [
                product(jnp.where(tris[d] > 0, att[a], 0.0), x_ref[0, d, c, a]) for a in range(2)
            ]
            y0 = jnp.where(left, ya, yb)
            qx = rq * jnp.exp(mid) + pltpu.roll(jnp.where(left, yb, ya), H, 1)
            if ci > 0:
                up_i = jnp.where(left, u, 0.0)
                ub_i = jnp.where(row < H, up_i, pltpu.roll(up_i, H, 1))
                up_t = jnp.where(left, 0.0, u)
                ub_t = jnp.where(row < H, pltpu.roll(up_t, H, 1), up_t)
                bh, bl = split2(jnp.concatenate([ub_i, ub_t], 1))
                q3 = left3(qx)
                qd = jnp.dot(
                    q3, jnp.concatenate([bh, bh], 0), preferred_element_type=F32
                ) + jnp.dot(q3[:, :C], bl, preferred_element_type=F32)
                y0 = y0 + qd[:, :C]
                qx = qd[:, C:]
            y_ref[d, sl, :] = y0
            qx_ref[d, sl, :] = qx


def layout(qkv, tokens):
    rows, width3 = qkv.shape
    width = width3 // 3
    seqs, hps, chunks = rows // tokens, width // 128, tokens // C
    part = lambda off: pl.BlockSpec((tokens, 128), lambda s, h: (s, h + off * hps))
    specs = dict(
        q=part(0),
        k=part(1),
        v=part(2),
        low=pl.BlockSpec((tokens, 256), lambda s, h: (s, 0)),
        x=pl.BlockSpec((1, 2, chunks, 2, C, 128), lambda s, h: (s * hps + h, 0, 0, 0, 0, 0)),
        u=pl.BlockSpec((1, 2, C, 128), lambda s, h: (s * hps + h, 0, 0, 0)),
        y=pl.BlockSpec((2, tokens, 128), lambda s, h: (0, s, h)),
        out=part(0),
    )
    return rows, width, seqs, hps, chunks, specs


def whole(*arrays):
    return [pl.BlockSpec(a.shape, lambda *i, n=a.ndim: (0,) * n) for a in arrays]


BIG = pltpu.CompilerParams(vmem_limit_bytes=56 * 1024 * 1024)


def maps(role, qkv, low, up, floor, par, tokens):
    _, width, seqs, hps, chunks, _ = layout(qkv, tokens)
    return pl.pallas_call(
        functools.partial(maps_kernel, role),
        grid=(seqs,),
        in_specs=[
            pl.BlockSpec((tokens, width), lambda s: (s, 1)),
            pl.BlockSpec((tokens, width), lambda s: (s, 2)),
            pl.BlockSpec((tokens, 256), lambda s: (s, 0)),
            *whole(up, floor, par),
        ],
        out_specs=[
            pl.BlockSpec((4 * hps, H, 128), lambda s: (s, 0, 0)),
            pl.BlockSpec((hps, 2, chunks, 2, C, 128), lambda s: (s, 0, 0, 0, 0, 0)),
            pl.BlockSpec((hps, 2, C, 128), lambda s: (s, 0, 0, 0)),
        ],
        out_shape=[
            jax.ShapeDtypeStruct((seqs * hps * 4, H, 128), BF),
            jax.ShapeDtypeStruct((seqs * hps, 2, chunks, 2, C, 128), F32),
            jax.ShapeDtypeStruct((seqs * hps, 2, C, 128), F32),
        ],
        compiler_params=BIG,
        cost_estimate=pl.CostEstimate(flops=8_000_000_000, bytes_accessed=6_000_000, transcendentals=0),
        name="maps",
    )(qkv, qkv, low, up, floor, par)


def outputs(role, qkv, low, up, floor, par, x, u, tokens):
    rows, width, seqs, hps, _, sp = layout(qkv, tokens)
    return pl.pallas_call(
        functools.partial(outputs_kernel, role),
        grid=(seqs, hps),
        in_specs=[
            sp["q"], sp["k"], sp["v"], sp["low"], *whole(up, floor, par), sp["x"], sp["u"]
        ],
        out_specs=[sp["y"], sp["y"], sp["out"]],
        out_shape=[
            jax.ShapeDtypeStruct((2, rows, width), F32),
            jax.ShapeDtypeStruct((2, rows, width), F32),
            jax.ShapeDtypeStruct((rows, width), F32),
        ],
        compiler_params=BIG,
        cost_estimate=pl.CostEstimate(flops=4_000_000_000, bytes_accessed=8_000_000, transcendentals=0),
        name="outputs",
    )(qkv, qkv, qkv, low, up, floor, par, x, u)


def final_kernel(role, y_ref, qx_ref, s_ref, own_ref, par_ref, o_ref):
    mean = head_ones(1.0 / H)
    z = jnp.zeros((H, H), BF)
    hps = own_ref.shape[1] // 128
    for hp in range(hps):
        ln = slice(hp * 128, (hp + 1) * 128)
        total = own_ref[:, ln]
        gain = head_row(par_ref, role() * hps + hp, 4)
        for d in range(2):
            sa, sb = s_ref[4 * hp + d], s_ref[4 * hp + 2 + d]
            blk = jnp.concatenate(
                [
                    jnp.concatenate([jnp.concatenate([sa[:, :H], sa[:, H:]], 0), z], 1),
                    jnp.concatenate([z, jnp.concatenate([sb[:, :H], sb[:, H:]], 0)], 1),
                ],
                0,
            )
            y = y_ref[d, :, ln] + jnp.dot(
                left3(qx_ref[d, :, ln]), jnp.concatenate([blk, blk], 0), preferred_element_type=F32
            )
            cen = y - head_sum(y, mean)
            var = head_sum(cen * cen, mean)
            total = total + cen * lax.rsqrt(var + 0.00064) * gain
        o_ref[:, ln] = total.astype(BF)


def final(role, y, qx, s, own, par, tokens):
    rows, width = own.shape
    hps = width // 128
    dspec = pl.BlockSpec((2, tokens, width), lambda s: (0, s, 0))
    one = pl.BlockSpec((tokens, width), lambda s: (s, 0))
    return pl.pallas_call(
        functools.partial(final_kernel, role),
        grid=(rows // tokens,),
        in_specs=[
            dspec,
            dspec,
            pl.BlockSpec((4 * hps, 32, 128), lambda s: (s, 0, 0)),
            one,
            *whole(par),
        ],
        out_specs=one,
        out_shape=jax.ShapeDtypeStruct((rows, width), BF),
        compiler_params=BIG,
        name="final",
    )(y, qx, s, own, par)


def scan_kernel(roles, back_of, u_ref, o_ref):
    groups = u_ref.shape[0] // roles
    back = back_of()
    states = [jnp.zeros((H, H), F32) for _ in range(roles)]
    zero = jnp.zeros((H, 128), BF)
    for i in range(groups):
        g = jnp.where(back == 1, groups - 1 - i, i)
        for p in range(roles):
            src = g * roles + p
            s = states[p]
            hi, lo = split2(s)
            o_ref[src] = jnp.concatenate([hi[:32], hi[32:]], 1)
            u = u_ref[src]
            t = jnp.dot(
                u, jnp.concatenate([zero, jnp.concatenate([hi, lo], 1)], 0), preferred_element_type=F32
            )
            states[p] = u[:, :H].astype(F32) + t[:, :H] + t[:, H:]


def scan_states(u, back, roles):
    n = u.shape[0]
    return pl.pallas_call(
        functools.partial(scan_kernel, roles, back),
        in_specs=[pl.BlockSpec(memory_space=pltpu.VMEM)],
        out_specs=pl.BlockSpec(memory_space=pltpu.VMEM),
        out_shape=jax.ShapeDtypeStruct((n, 32, 128), BF),
        name="states",
    )(u)


def place():
    z, dp = lax.axis_index("sp"), lax.axis_index("dp")
    j = dp // 2
    return z % 2, dp % 2, j // 4, j % 4


def role():
    p, c, _, _ = place()
    return 2 * p + c


def backwards():
    return lax.axis_index("sp") % 2


def project_kernel(b0, fm, fp, fo, r1, r2, r3t, r3b, t0, t1, t2, t3, qkv_ref, low_ref, w_ref, t_ref, sem):
    p, c, y, x = place()
    rows = b0.shape[0]
    n = t0.shape[0]
    a = jnp.where(c == 0, x, y)
    b = jnp.where(c == 0, y, x)
    copies = []

    def move(src, dst):
        cp = pltpu.make_async_copy(src, dst, sem.at[len(copies)])
        cp.start()
        copies.append(cp)

    for i, t in enumerate((t0, t1, t2, t3)):
        at = 2 * (c if i < 2 else 1 - c) + (p if i % 2 == 0 else 1 - p)
        move(t, t_ref.at[pl.ds(pl.multiple_of(at * n, n), n)])
    for eps, parts in (
        (0, [(b0, 0), (fm, 0), (fp, 0), (fo, 0)]),
        (-1, [(r1, i) for i in range(4)]),
        (1, [(r2, i) for i in range(4)]),
        (2, [(r3t, 0), (r3t, 1), (r3b, 0), (r3b, 1)]),
    ):
        for delta, (ref, i) in zip((0, -1, 1, 2), parts):
            aa, bb = lax.rem(a + delta + 4, 4), lax.rem(b + eps + 4, 4)
            chip = jnp.where(c == 0, bb * 4 + aa, aa * 4 + bb)
            move(ref.at[pl.ds(i * rows, rows)], w_ref.at[chip])
    for cp in copies:
        cp.wait()
    width3 = qkv_ref.shape[1]
    out = jnp.dot(t_ref[...], w_ref[...].reshape(-1, w_ref.shape[2]), preferred_element_type=F32)
    qkv_ref[...] = out[:, :width3].astype(BF)
    low_ref[...] = jnp.tanh(out[:, width3:]).astype(BF)


def project(blocks, toks, width3):
    rows, cols = blocks[0].shape
    n, depth = toks[0].shape
    vm = pl.BlockSpec(memory_space=pltpu.VMEM)
    return pl.pallas_call(
        project_kernel,
        in_specs=[pl.BlockSpec(memory_space=pl.ANY)] * 12,
        out_specs=[vm, vm],
        out_shape=[
            jax.ShapeDtypeStruct((4 * n, width3), BF),
            jax.ShapeDtypeStruct((4 * n, cols - width3), BF),
        ],
        scratch_shapes=[
            pltpu.VMEM((16, rows, cols), BF),
            pltpu.VMEM((4 * n, depth), BF),
            pltpu.SemaphoreType.DMA((20,)),
        ],
        compiler_params=BIG,
        name="project",
    )(*blocks, *toks)


def shift(first, by):
    pairs = []
    for i in range(32):
        core, j = i % 2, i // 2
        y, x = j // 4, j % 4
        if (core == 0) == first:
            x = (x + by) % 4
        else:
            y = (y + by) % 4
        pairs.append((i, (y * 4 + x) * 2 + core))
    return pairs


CORES = [(i, i ^ 1) for i in range(32)]
ZPAIRS = [(i, i ^ 1) for i in range(16)]


def body(tokens, wq, wk, wv, wd, up, floor, rate, diag, gain):
    p, c, _, _ = place()
    width = 256
    tok = tokens.reshape(-1, tokens.shape[2])
    n = tok.shape[0]

    def columns(r):
        cut = lambda w: lax.dynamic_slice_in_dim(w, r * width, width, 1)
        return jnp.concatenate([cut(wq), cut(wk), cut(wv), wd], 1)

    keep = columns(2 * p + c)
    recv = lax.ppermute(columns(2 * p + 1 - c), "dp", CORES)
    b0 = jnp.where(c == 0, jnp.concatenate([keep, recv], 0), jnp.concatenate([recv, keep], 0))
    rows = b0.shape[0]
    fm = lax.ppermute(b0, "dp", shift(True, 1))
    fp = lax.ppermute(b0, "dp", shift(True, -1))
    fo = lax.ppermute(b0, "dp", shift(True, 2))
    tz = lax.ppermute(tok, "sp", ZPAIRS)
    tc = lax.ppermute(tok, "dp", CORES)
    s4 = jnp.concatenate([b0, fm, fp, fo], 0)

    par = jnp.concatenate([rate, diag, gain[None], jnp.zeros((3, gain.shape[0]), F32)], 0)
    par = jnp.broadcast_to(par[None], (16,) + par.shape)
    par = lax.all_to_all(par, "sp", split_axis=0, concat_axis=0, tiled=True)
    r1 = lax.ppermute(s4, "dp", shift(False, 1))
    r2 = lax.ppermute(s4, "dp", shift(False, -1))
    tcz = lax.ppermute(tz, "dp", CORES)
    r3t = lax.ppermute(r1[: 2 * rows], "dp", shift(False, 1))
    r3b = lax.ppermute(r2[2 * rows :], "dp", shift(False, -1))
    qkv, low = project((b0, fm, fp, fo, r1, r2, r3t, r3b), (tok, tz, tc, tcz), 3 * width)
    span = 2 * n
    msg, xs, us = maps(role, qkv, low, up, floor, par, span)
    got = lax.all_to_all(msg, "sp", split_axis=0, concat_axis=0, tiled=True)
    y0, qx, own = outputs(role, qkv, low, up, floor, par, xs, us, span)
    st = scan_states(got, backwards, 2)
    st = lax.all_to_all(st, "sp", split_axis=0, concat_axis=0, tiled=True)
    out = final(role, y0, qx, st, own, par, span)

    out = out.reshape(2, 2, n, width)
    mine = lax.dynamic_index_in_dim(out, p, 1, False)
    rz = lax.ppermute(lax.dynamic_index_in_dim(out, 1 - p, 1, False), "sp", ZPAIRS)
    pick = lambda m, s: lax.dynamic_index_in_dim(m, s, 0, False)
    low_p = jnp.where(p == 0, mine, rz)
    high_p = jnp.where(p == 0, rz, mine)
    both = jnp.concatenate([low_p, high_p], 2)
    far = lax.ppermute(pick(both, 1 - c), "dp", CORES)
    near = pick(both, c)
    first = jnp.where(c == 0, near, far)
    second = jnp.where(c == 0, far, near)
    res = jnp.concatenate(
        [first[:, :width], second[:, :width], first[:, width:], second[:, width:]], 1
    )
    return res.reshape(1, n, 4 * width)


def solution(mesh):
    in_specs = (
        P("dp", "sp", None),
        P("dp", None),
        P("dp", None),
        P("dp", None),
        P("dp", None),
        P(),
        P(),
        P(None, "sp"),
        P(None, "sp"),
        P("sp"),
    )
    return jax.shard_map(
        body, mesh=mesh, in_specs=in_specs, out_specs=P("dp", "sp", None), check_vma=False
    )
```

```python
import math
import functools
import jax
import jax.numpy as jnp
from jax import lax
from jax.experimental import pallas as pl
from jax.experimental.pallas import tpu as pltpu
from jax.sharding import PartitionSpec as P

BF = jnp.bfloat16
F32 = jnp.float32
C = 128
H = 64


def split2(x):
    hi = x.astype(BF)
    return hi, (x - hi.astype(F32)).astype(BF)


def left3(a):
    hi, lo = split2(a)
    return jnp.concatenate([hi, lo], 1)


def right3(b):
    hi, lo = split2(b)
    return jnp.concatenate(
        [jnp.concatenate([hi, lo], 1), jnp.concatenate([hi, jnp.zeros_like(lo)], 1)], 0
    )


def dot3(a3, b3):
    t = jnp.dot(a3, b3, preferred_element_type=F32)
    n = t.shape[1] // 2
    return t[:, :n] + t[:, n:]


def nt(a, b):
    return lax.dot_general(a, b, (((1,), (1,)), ((), ())), preferred_element_type=F32)


def tn(a, b):
    return lax.dot_general(a, b, (((0,), (0,)), ((), ())), preferred_element_type=F32)


def head_ones(scale=1.0):
    r = lax.broadcasted_iota(jnp.int32, (256, 128), 0)
    c = lax.broadcasted_iota(jnp.int32, (256, 128), 1)
    return jnp.where(((r >> 6) & 1) == (c >> 6), scale, 0.0).astype(BF)


def head_sum(x, ones):
    hi, lo = split2(x)
    return jnp.dot(jnp.concatenate([hi, lo], 1), ones, preferred_element_type=F32)


def mm(a, b):
    return jnp.dot(a.astype(BF), b.astype(BF), preferred_element_type=F32)


def product(a, b):
    return dot3(left3(a), right3(b))


def pick_rows(x, size, off):
    return jnp.concatenate([x[i + off : i + off + size] for i in range(0, C, 2 * size)], 0)


def put_rows(rows, rest, size, off):
    parts = []
    for n, i in enumerate(range(0, C, 2 * size)):
        new = rows[n * size : (n + 1) * size]
        old = rest[i : i + size] if off else rest[i + size : i + 2 * size]
        parts += [old, new] if off else [new, old]
    return jnp.concatenate(parts, 0)


def gates(d, low, up, floor, pair):
    lanes = pl.ds(pl.multiple_of(pair * 128, 128), 128)
    pre = (
        jnp.dot(low[:, d * 128 : (d + 1) * 128], up[d, :, lanes], preferred_element_type=F32)
        + floor[d : d + 1, lanes]
    )
    return -math.exp(-0.5) * jax.nn.sigmoid(pre.astype(BF).astype(F32))


def head_row(par, pair, i):
    return jnp.concatenate([par[2 * pair, i : i + 1, :], par[2 * pair + 1, i : i + 1, :]], 1)


def sums(d, ld, tri):
    hi, lo = split2(ld)
    cs = jnp.dot(tri, jnp.concatenate([hi, lo], 1), preferred_element_type=F32)
    inc = cs[:, :128] + cs[:, 128:]
    return inc, inc[C // 2 : C // 2 + 1], inc[C - 1 : C] if d == 0 else inc[0:1]


def against(parts, pk):
    pkh, pkl = split2(pk)
    rhs = jnp.concatenate(
        [jnp.concatenate([pkh, pkh], 1), jnp.concatenate([pkl, jnp.zeros_like(pkl)], 1)], 0
    )
    att = nt(jnp.concatenate([left3(p) for p in parts], 0), rhs)
    att = att[:, :C] + att[:, C:]
    return [att[i * C : (i + 1) * C] for i in range(len(parts))]


def consts():
    row = lax.broadcasted_iota(jnp.int32, (C, C), 0)
    col = lax.broadcasted_iota(jnp.int32, (C, C), 1)
    tris = [jnp.where(m, 1.0, 0.0).astype(BF) for m in (col <= row, col >= row)]
    return row, col, row ^ col, col < H, tris


def maps_kernel(role, k_ref, v_ref, low_ref, up_ref, floor_ref, par_ref, msg_ref, x_ref, u_ref):
    chunks = k_ref.shape[0] // C
    row, col, x, left, tris = consts()
    hps = k_ref.shape[1] // 128
    probs = []
    for hp, d in [(hp, d) for hp in range(hps) for d in range(2)]:
        ln = slice(hp * 128, (hp + 1) * 128)
        k = k_ref[:, ln].astype(F32)
        v = v_ref[:, ln].astype(F32)
        nk = -(k / (1.0 + head_sum(k * k, head_ones())))
        pair = role() * hps + hp
        logd = gates(d, low_ref, up_ref, floor_ref, pair)
        kap = k * jax.nn.sigmoid(head_row(par_ref, pair, d))
        strict = (col < row) if d == 0 else (col > row)
        for ci in range(chunks):
            c = ci if d == 0 else chunks - 1 - ci
            sl = slice(c * C, (c + 1) * C)
            ld = logd[sl]
            inc, mid, fin = sums(d, ld, tris[d])
            rel = inc - mid
            gq = nk[sl] * jnp.exp(rel - ld)
            pk = kap[sl] * jnp.exp(-rel)
            ke = pk * jnp.exp(fin - mid)
            gl = pltpu.roll(gq * jnp.exp(mid), H, 1)
            vs = v[sl]
            zero = jnp.zeros_like(gq)
            att = against([jnp.where(left, gq, zero), jnp.where(left, zero, gq)], pk)
            heads = []
            for a in range(2):
                m = jnp.where(strict, att[a], 0.0)
                b = jnp.where(left, vs, gl) if a == 0 else jnp.where(left, gl, vs)
                heads.append(dict(m=m, b=b, d=d))
            probs.append(dict(d=d, c=c, heads=heads, ke=ke, fin=fin))
    allh = [h for p in probs for h in p["heads"]]
    zero = jnp.zeros((C, C), F32)
    for h in allh:
        h["n"] = jnp.where(x == 1, h["m"], 0.0)
    for lb in range(1, 7):
        size = 1 << lb
        sel = (x >> lb) == 1
        for h in allh:
            off = jnp.where(sel, h["m"], 0.0)
            if size >= 8:
                at = size if h["d"] == 0 else 0
                off = pick_rows(off, size, at)
                h["w"] = off + mm(off, h["n"])
            else:
                h["w"] = off + mm(off, h["n"])
        for h in allh:
            if size >= 8:
                at = size if h["d"] == 0 else 0
                nr = pick_rows(h["n"], size, at)
                nr = nr + h["w"] + mm(nr, put_rows(h["w"], zero, size, at))
                h["n"] = put_rows(nr, h["n"], size, at)
            else:
                h["n"] = h["n"] + h["w"] + mm(h["n"], h["w"])
    for h in allh:
        h["nb"] = h["n"].astype(BF)
        h["x"] = h["b"] + mm(h["nb"], h["b"])
    for h in allh:
        h["res"] = h["b"] - h["x"] + product(h["m"], h["x"])
    for h in allh:
        h["x"] = h["x"] + h["res"] + mm(h["nb"], h["res"])
    for hp, d in [(hp, d) for hp in range(hps) for d in range(2)]:
        u = None
        for ci in range(chunks):
            p = probs[(hp * 2 + d) * chunks + ci]
            xa, xb = p["heads"][0]["x"], p["heads"][1]["x"]
            x_ref[hp, d, p["c"], 0] = xa
            x_ref[hp, d, p["c"], 1] = xb
            kh, kl = split2(
                jnp.concatenate([jnp.where(left, p["ke"], 0.0), jnp.where(left, 0.0, p["ke"])], 0)
            )
            xh, xl = split2(jnp.concatenate([xa, xb], 0))
            un = tn(kh, jnp.concatenate([xh, xl], 1))
            un = un[:, :C] + un[:, C:] + tn(kl, xh)
            un = jnp.where(row < H, un, pltpu.roll(un, H, 1))
            ef = jnp.broadcast_to(jnp.exp(p["fin"]), (C, C))
            dm = jnp.where(row < H, pltpu.roll(ef, H, 1), ef)
            un = un + jnp.where(col == (row & (H - 1)) + H, dm, 0.0)
            if u is None:
                u = un
                u_ref[hp, d] = u
            else:
                t2 = jnp.where(
                    row < H,
                    jnp.where(left, pltpu.roll(un, H, 1), 0.0),
                    jnp.where(left, 0.0, un),
                )
                u = product(t2, u) + jnp.where(left, un, 0.0)
        msg_ref[4 * hp + d] = u[:H].astype(BF)
        msg_ref[4 * hp + 2 + d] = u[H:].astype(BF)


def outputs_kernel(
    role, q_ref, k_ref, v_ref, low_ref, up_ref, floor_ref, par_ref, x_ref, u_ref, y_ref, qx_ref, own_ref
):
    chunks = k_ref.shape[0] // C
    q = q_ref[...].astype(F32)
    k = k_ref[...].astype(F32)
    row, _, _, left, tris = consts()
    pair = role() * pl.num_programs(1) + pl.program_id(1)
    rates = [jax.nn.sigmoid(head_row(par_ref, pair, d)) for d in range(2)]
    wt = rates[0] * head_row(par_ref, pair, 2) + rates[1] * head_row(par_ref, pair, 3)
    own_ref[...] = head_sum(q * k * wt, head_ones()) * v_ref[...].astype(F32)
    for d in range(2):
        logd = gates(d, low_ref, up_ref, floor_ref, pair)
        kap = k * rates[d]
        u = u_ref[0, d]
        for ci in range(chunks):
            c = ci if d == 0 else chunks - 1 - ci
            sl = slice(c * C, (c + 1) * C)
            inc, mid, _ = sums(d, logd[sl], tris[d])
            rel = inc - mid
            rq = q[sl] * jnp.exp(rel)
            pk = kap[sl] * jnp.exp(-rel)
            zero = jnp.zeros_like(rq)
            att = against([jnp.where(left, rq, zero), jnp.where(left, zero, rq)], pk)
            ya, yb = [
                product(jnp.where(tris[d] > 0, att[a], 0.0), x_ref[0, d, c, a]) for a in range(2)
            ]
            y0 = jnp.where(left, ya, yb)
            qx = rq * jnp.exp(mid) + pltpu.roll(jnp.where(left, yb, ya), H, 1)
            if ci > 0:
                up_i = jnp.where(left, u, 0.0)
                ub_i = jnp.where(row < H, up_i, pltpu.roll(up_i, H, 1))
                up_t = jnp.where(left, 0.0, u)
                ub_t = jnp.where(row < H, pltpu.roll(up_t, H, 1), up_t)
                bh, bl = split2(jnp.concatenate([ub_i, ub_t], 1))
                q3 = left3(qx)
                qd = jnp.dot(
                    q3, jnp.concatenate([bh, bh], 0), preferred_element_type=F32
                ) + jnp.dot(q3[:, :C], bl, preferred_element_type=F32)
                y0 = y0 + qd[:, :C]
                qx = qd[:, C:]
            y_ref[d, sl, :] = y0
            qx_ref[d, sl, :] = qx


def layout(qkv, tokens):
    rows, width3 = qkv.shape
    width = width3 // 3
    seqs, hps, chunks = rows // tokens, width // 128, tokens // C
    part = lambda off: pl.BlockSpec((tokens, 128), lambda s, h: (s, h + off * hps))
    specs = dict(
        q=part(0),
        k=part(1),
        v=part(2),
        low=pl.BlockSpec((tokens, 256), lambda s, h: (s, 0)),
        x=pl.BlockSpec((1, 2, chunks, 2, C, 128), lambda s, h: (s * hps + h, 0, 0, 0, 0, 0)),
        u=pl.BlockSpec((1, 2, C, 128), lambda s, h: (s * hps + h, 0, 0, 0)),
        y=pl.BlockSpec((2, tokens, 128), lambda s, h: (0, s, h)),
        out=part(0),
    )
    return rows, width, seqs, hps, chunks, specs


def whole(*arrays):
    return [pl.BlockSpec(a.shape, lambda *i, n=a.ndim: (0,) * n) for a in arrays]


BIG = pltpu.CompilerParams(vmem_limit_bytes=56 * 1024 * 1024)


def maps(role, qkv, low, up, floor, par, tokens):
    _, width, seqs, hps, chunks, _ = layout(qkv, tokens)
    return pl.pallas_call(
        functools.partial(maps_kernel, role),
        grid=(seqs,),
        in_specs=[
            pl.BlockSpec((tokens, width), lambda s: (s, 1)),
            pl.BlockSpec((tokens, width), lambda s: (s, 2)),
            pl.BlockSpec((tokens, 256), lambda s: (s, 0)),
            *whole(up, floor, par),
        ],
        out_specs=[
            pl.BlockSpec((4 * hps, H, 128), lambda s: (s, 0, 0)),
            pl.BlockSpec((hps, 2, chunks, 2, C, 128), lambda s: (s, 0, 0, 0, 0, 0)),
            pl.BlockSpec((hps, 2, C, 128), lambda s: (s, 0, 0, 0)),
        ],
        out_shape=[
            jax.ShapeDtypeStruct((seqs * hps * 4, H, 128), BF),
            jax.ShapeDtypeStruct((seqs * hps, 2, chunks, 2, C, 128), F32),
            jax.ShapeDtypeStruct((seqs * hps, 2, C, 128), F32),
        ],
        compiler_params=BIG,
        cost_estimate=pl.CostEstimate(flops=8_000_000_000, bytes_accessed=6_000_000, transcendentals=0),
        name="maps",
    )(qkv, qkv, low, up, floor, par)


def outputs(role, qkv, low, up, floor, par, x, u, tokens):
    rows, width, seqs, hps, _, sp = layout(qkv, tokens)
    return pl.pallas_call(
        functools.partial(outputs_kernel, role),
        grid=(seqs, hps),
        in_specs=[
            sp["q"], sp["k"], sp["v"], sp["low"], *whole(up, floor, par), sp["x"], sp["u"]
        ],
        out_specs=[sp["y"], sp["y"], sp["out"]],
        out_shape=[
            jax.ShapeDtypeStruct((2, rows, width), F32),
            jax.ShapeDtypeStruct((2, rows, width), F32),
            jax.ShapeDtypeStruct((rows, width), F32),
        ],
        compiler_params=BIG,
        cost_estimate=pl.CostEstimate(flops=4_000_000_000, bytes_accessed=8_000_000, transcendentals=0),
        name="outputs",
    )(qkv, qkv, qkv, low, up, floor, par, x, u)


def final_kernel(place, y_ref, qx_ref, s_ref, own_ref, par_ref, here, along, across, both, o_ref):
    mean = head_ones(1.0 / H)
    z = jnp.zeros((H, H), BF)
    hps = own_ref.shape[1] // 128
    p, c, _, _ = place()
    seq = pl.program_id(0)
    for hp in range(hps):
        ln = slice(hp * 128, (hp + 1) * 128)
        total = own_ref[:, ln]
        gain = head_row(par_ref, (2 * p + c) * hps + hp, 4)
        for d in range(2):
            sa, sb = s_ref[4 * hp + d], s_ref[4 * hp + 2 + d]
            blk = jnp.concatenate(
                [
                    jnp.concatenate([jnp.concatenate([sa[:, :H], sa[:, H:]], 0), z], 1),
                    jnp.concatenate([z, jnp.concatenate([sb[:, :H], sb[:, H:]], 0)], 1),
                ],
                0,
            )
            y = y_ref[d, :, ln] + jnp.dot(
                left3(qx_ref[d, :, ln]), jnp.concatenate([blk, blk], 0), preferred_element_type=F32
            )
            cen = y - head_sum(y, mean)
            var = head_sum(cen * cen, mean)
            total = total + cen * lax.rsqrt(var + 0.00064) * gain
        o_ref[seq, :, :, ln] = total.astype(BF).reshape(2, -1, 128)

    @pl.when(seq == 1)
    def _():
        here[...] = o_ref[c, p]
        along[...] = o_ref[c, 1 - p]
        across[...] = o_ref[1 - c, p]
        both[...] = o_ref[1 - c, 1 - p]


def final(place, y, qx, s, own, par, tokens):
    rows, width = own.shape
    hps = width // 128
    dspec = pl.BlockSpec((2, tokens, width), lambda s: (0, s, 0))
    one = pl.BlockSpec((tokens, width), lambda s: (s, 0))
    return pl.pallas_call(
        functools.partial(final_kernel, place),
        grid=(rows // tokens,),
        in_specs=[
            dspec,
            dspec,
            pl.BlockSpec((4 * hps, 32, 128), lambda s: (s, 0, 0)),
            one,
            *whole(par),
        ],
        out_specs=[pl.BlockSpec((tokens // 2, width), lambda s: (0, 0))] * 4,
        out_shape=[jax.ShapeDtypeStruct((tokens // 2, width), BF)] * 4,
        scratch_shapes=[pltpu.VMEM((2, 2, tokens // 2, width), BF)],
        compiler_params=BIG,
        name="final",
    )(y, qx, s, own, par)


def scan_kernel(roles, back_of, u_ref, o_ref):
    groups = u_ref.shape[0] // roles
    back = back_of()
    states = [jnp.zeros((H, H), F32) for _ in range(roles)]
    zero = jnp.zeros((H, 128), BF)
    for i in range(groups):
        g = jnp.where(back == 1, groups - 1 - i, i)
        for p in range(roles):
            src = g * roles + p
            s = states[p]
            hi, lo = split2(s)
            o_ref[src] = jnp.concatenate([hi[:32], hi[32:]], 1)
            u = u_ref[src]
            t = jnp.dot(
                u, jnp.concatenate([zero, jnp.concatenate([hi, lo], 1)], 0), preferred_element_type=F32
            )
            states[p] = u[:, :H].astype(F32) + t[:, :H] + t[:, H:]


def scan_states(u, back, roles):
    n = u.shape[0]
    return pl.pallas_call(
        functools.partial(scan_kernel, roles, back),
        in_specs=[pl.BlockSpec(memory_space=pltpu.VMEM)],
        out_specs=pl.BlockSpec(memory_space=pltpu.VMEM),
        out_shape=jax.ShapeDtypeStruct((n, 32, 128), BF),
        name="states",
    )(u)


def place():
    z, dp = lax.axis_index("sp"), lax.axis_index("dp")
    j = dp // 2
    return z % 2, dp % 2, j // 4, j % 4


def role():
    p, c, _, _ = place()
    return 2 * p + c


def backwards():
    return lax.axis_index("sp") % 2


def project_kernel(b0, fm, fp, fo, r1, r2, ro, t0, t1, t2, t3, qkv_ref, low_ref, w_ref, t_ref, sem):
    p, c, y, x = place()
    rows = b0.shape[0]
    n = t0.shape[0]
    a = jnp.where(c == 0, x, y)
    b = jnp.where(c == 0, y, x)
    copies = []

    def move(src, dst):
        cp = pltpu.make_async_copy(src, dst, sem.at[len(copies)])
        cp.start()
        copies.append(cp)

    for i, t in enumerate((t0, t1, t2, t3)):
        at = 2 * (c if i < 2 else 1 - c) + (p if i % 2 == 0 else 1 - p)
        move(t, t_ref.at[pl.ds(pl.multiple_of(at * n, n), n)])
    for eps, parts in (
        (0, [(b0, 0), (fm, 0), (fp, 0), (fo, 0)]),
        (-1, [(r1, i) for i in range(4)]),
        (1, [(r2, i) for i in range(4)]),
        (2, [(ro, i) for i in range(4)]),
    ):
        for delta, (ref, i) in zip((0, -1, 1, 2), parts):
            aa, bb = lax.rem(a + delta + 4, 4), lax.rem(b + eps + 4, 4)
            chip = jnp.where(c == 0, bb * 4 + aa, aa * 4 + bb)
            move(ref.at[pl.ds(i * rows, rows)], w_ref.at[chip])
    for cp in copies:
        cp.wait()
    width3 = qkv_ref.shape[1]
    out = jnp.dot(t_ref[...], w_ref[...].reshape(-1, w_ref.shape[2]), preferred_element_type=F32)
    qkv_ref[...] = out[:, :width3].astype(BF)
    low_ref[...] = jnp.tanh(out[:, width3:]).astype(BF)


def project(blocks, toks, width3):
    rows, cols = blocks[0].shape
    n, depth = toks[0].shape
    vm = pl.BlockSpec(memory_space=pltpu.VMEM)
    return pl.pallas_call(
        project_kernel,
        in_specs=[pl.BlockSpec(memory_space=pl.ANY)] * 11,
        out_specs=[vm, vm],
        out_shape=[
            jax.ShapeDtypeStruct((4 * n, width3), BF),
            jax.ShapeDtypeStruct((4 * n, cols - width3), BF),
        ],
        scratch_shapes=[
            pltpu.VMEM((16, rows, cols), BF),
            pltpu.VMEM((4 * n, depth), BF),
            pltpu.SemaphoreType.DMA((20,)),
        ],
        compiler_params=BIG,
        name="project",
    )(*blocks, *toks)


def shift(first, by):
    pairs = []
    for i in range(32):
        core, j = i % 2, i // 2
        y, x = j // 4, j % 4
        if (core == 0) == first:
            x = (x + by) % 4
        else:
            y = (y + by) % 4
        pairs.append((i, (y * 4 + x) * 2 + core))
    return pairs


CORES = [(i, i ^ 1) for i in range(32)]
ZPAIRS = [(i, i ^ 1) for i in range(16)]


def body(tokens, wq, wk, wv, wd, up, floor, rate, diag, gain):
    p, c, _, _ = place()
    width = 256
    tok = tokens.reshape(-1, tokens.shape[2])
    n = tok.shape[0]

    def columns(r):
        cut = lambda w: lax.dynamic_slice_in_dim(w, r * width, width, 1)
        return jnp.concatenate([cut(wq), cut(wk), cut(wv), wd], 1)

    keep = columns(2 * p + c)
    recv = lax.ppermute(columns(2 * p + 1 - c), "dp", CORES)
    b0 = jnp.where(c == 0, jnp.concatenate([keep, recv], 0), jnp.concatenate([recv, keep], 0))
    fm = lax.ppermute(b0, "dp", shift(True, 1))
    fp = lax.ppermute(b0, "dp", shift(True, -1))
    fo = lax.ppermute(b0, "dp", shift(True, 2))
    tz = lax.ppermute(tok, "sp", ZPAIRS)
    tc = lax.ppermute(tok, "dp", CORES)
    s4 = jnp.concatenate([b0, fm, fp, fo], 0)

    par = jnp.concatenate([rate, diag, gain[None], jnp.zeros((3, gain.shape[0]), F32)], 0)
    par = jnp.broadcast_to(par[None], (16,) + par.shape)
    par = lax.all_to_all(par, "sp", split_axis=0, concat_axis=0, tiled=True)
    r1 = lax.ppermute(s4, "dp", shift(False, 1))
    r2 = lax.ppermute(s4, "dp", shift(False, -1))
    ro = lax.ppermute(s4, "dp", shift(False, 2))
    tcz = lax.ppermute(tz, "dp", CORES)
    qkv, low = project((b0, fm, fp, fo, r1, r2, ro), (tok, tz, tc, tcz), 3 * width)
    span = 2 * n
    msg, xs, us = maps(role, qkv, low, up, floor, par, span)
    got = lax.all_to_all(msg, "sp", split_axis=0, concat_axis=0, tiled=True)
    y0, qx, own = outputs(role, qkv, low, up, floor, par, xs, us, span)
    st = scan_states(got, backwards, 2)
    st = lax.all_to_all(st, "sp", split_axis=0, concat_axis=0, tiled=True)
    here, along, across, both = final(place, y0, qx, st, own, par, span)
    both = lax.ppermute(
        both, ("sp", "dp"), [(32 * i + k, 32 * (i ^ 1) + (k ^ 1)) for i in range(16) for k in range(32)]
    )
    along = lax.ppermute(along, "sp", ZPAIRS)
    across = lax.ppermute(across, "dp", CORES)
    low = [jnp.where(p == 0, here, along), jnp.where(p == 0, across, both)]
    high = [jnp.where(p == 0, along, here), jnp.where(p == 0, both, across)]
    parts = []
    for m, o in (low, high):
        parts += [jnp.where(c == 0, m, o), jnp.where(c == 0, o, m)]
    res = jnp.concatenate(parts, 1)
    return res.reshape(1, n, 4 * width)


def solution(mesh):
    in_specs = (
        P("dp", "sp", None),
        P("dp", None),
        P("dp", None),
        P("dp", None),
        P("dp", None),
        P(),
        P(),
        P(None, "sp"),
        P(None, "sp"),
        P("sp"),
    )
    return jax.shard_map(
        body, mesh=mesh, in_specs=in_specs, out_specs=P("dp", "sp", None), check_vma=False
    )
```
